32 devices in a mesh: ep: 8 (over z, core), tp: 4 (over y, x).
Axes of the slice: x: 2, y: 2, z: 4, core: 2. Of those that a mesh axis runs over, the one named last changes fastest.
Arguments:
- tokens: bfloat16 [1024, 1024], P('ep', 'tp'), may hold values from -6 to 6
- norm_gain: float32 [1024], replicated, may hold values from 0.1 to 1.9
- gate_weight: bfloat16 [8, 1024, 1024], P('ep', None, 'tp'), may hold values from -0.1875 to 0.1875
- up_weight: bfloat16 [8, 1024, 1024], P('ep', None, 'tp'), may hold values from -0.1875 to 0.1875
- down_weight: bfloat16 [8, 1024, 1024], P('ep', None, 'tp'), may hold values from -0.1875 to 0.1875
- expert_ids: int32 [1024, 4], P('ep'), may hold values from 0 to 7, all different within a row; in each aligned block of 128 rows (0 to 127, 128 to 255, ...) at most 128 rows name the same one
- route_weight: float32 [1024, 4], P('ep'), may hold values from 0.2 to 1
Outputs:
- combined: bfloat16 [1024, 1024], P('ep', 'tp')
The draws below stay inside these ranges and needn't reach their ends.
Inputs may be any that keep to these rules, and one draw needn't show every extreme that they name: `expert_ids`: each token names 4 different experts; in each aligned block of 128 tokens no expert is named by more than 128 of them, and in some block one expert is named by exactly 128; every expert is named by some token.
All inputs are finite; a program needn't handle non-finite values.
Results may differ from the reference program's by a relative error of at most 0.0035.
Values may be sent and summed in bfloat16 or wider, within the bound.
A program may use at most 64 MiB of HBM per device.

```python
import math
import jax
import jax.numpy as jnp
import numpy as np
from jax import lax

D = 1024
FF = 1024
TOPK = 4
TOK_DEV = 128
EXPERTS = 8
TOKENS = 1024
CAP = 128
N_EP = 8


def level_of(key, shape, cuts, low, top_value):
    def one(position, blocks):
        heights = jax.random.uniform(jax.random.fold_in(jax.random.fold_in(key, 6), position), (blocks,), jnp.float32, low / len(cuts), top_value / len(cuts))
        return jnp.repeat(jnp.exp(heights), shape[position] // blocks).reshape((-1,) + (1,) * (len(shape) - position - 1))

    gain = one(*cuts[0])
    for cut in cuts[1:]:
        gain = gain * one(*cut)
    return gain


def deal_out(rng, own, number, rows, amount, top, bound, lean):
    order = jax.random.permutation(rng, amount)
    crowded, usual = shares(amount, rows * top, bound, lean, True), shares(amount, rows * top, bound, lean, False)
    places = jnp.arange(amount)

    def named(sizes, rotation):
        used = int((sizes > 0).sum())
        fixed = max(1, used // 4)
        passed = fixed + (places - fixed + rotation * (used - fixed)) % max(1, amount - fixed)
        return jnp.zeros((amount,), jnp.int32).at[order[jnp.where(places < fixed, places, passed)]].set(jnp.asarray(sizes, jnp.int32))

    sizes = jnp.where(number % 4 == 0, named(crowded, number // 4), named(usual, number - number // 4 - 1))
    mixed = jax.random.permutation(jax.random.fold_in(own, 3), amount)
    giver, taker = mixed[0:amount // 2 * 2:2], mixed[1:amount // 2 * 2:2]
    room = jnp.minimum(sizes[giver] - 1, bound - sizes[taker]) // 2
    room = jnp.where((giver == order[0]) | (taker == order[0]) | (sizes[taker] == 0), 0, jnp.maximum(room, 0))
    passed = jax.random.randint(jax.random.fold_in(own, 4), (amount // 2,), 0, 1 << 20) % (room + 1)
    sizes = sizes.at[giver].add(-passed).at[taker].add(passed)
    members = jnp.searchsorted(jnp.cumsum(sizes), jnp.arange(rows * top), side="right").astype(jnp.int32)
    grid = members.reshape(top, rows).T
    grid = grid[jax.random.permutation(jax.random.fold_in(own, 1), rows)]
    rotation = jax.random.randint(jax.random.fold_in(own, 2), (rows, 1), 0, top)
    return jnp.take_along_axis(grid, (jnp.arange(top)[None, :] + rotation) % top, axis=1)


def shares(number_of, total, most, slope, full):
    weights = [(1 << 20) // math.isqrt(grade ** slope) + 1 for grade in range(1, number_of + 1)]
    largest = most if full else min(most, max(-(-total // number_of), total * weights[0] // sum(weights)))
    least = 1 if total - largest >= number_of - 1 else 0
    given, rest = [largest] + [least] * (number_of - 1), total - largest - least * (number_of - 1)
    while rest > 0:
        free = [i for i in range(1, number_of) if given[i] < largest] or [i for i in range(1, number_of) if given[i] < most]
        pool, left = sum([weights[i] for i in free]), rest
        for i in free:
            extra = min(most - given[i], max(1, left * weights[i] // pool), rest)
            given[i] = given[i] + extra
            rest = rest - extra
    return np.array(given)


def noise(key, shape, scale, most, shards=(), held_as=jnp.bfloat16):
    array = scale * jax.random.normal(key, shape, jnp.float32)
    if shards:
        array = array * level_of(key, shape, shards, -0.22, 0.18)
    return jnp.clip(array, -most, most).astype(held_as)


def setup_inputs(seed: int = 0) -> dict:
    keys = jax.random.split(jax.random.key(seed), 8)
    tokens = noise(keys[0], (TOKENS, D), 1.0, 6.0, ((0, 8), (1, 4)))
    norm_gain = jnp.clip(1.0 + 0.18 * jax.random.normal(keys[1], (D,), jnp.float32), 0.1, 1.9)
    gate_weight = noise(keys[2], (EXPERTS, D, FF), D ** -0.5, 0.1875, ((0, 8), (2, 4)))
    up_weight = noise(keys[3], (EXPERTS, D, FF), D ** -0.5, 0.1875, ((0, 8), (2, 4)))
    down_weight = noise(keys[4], (EXPERTS, FF, D), FF ** -0.5, 0.1875, ((0, 8), (2, 4)))
    expert_ids_keys = jax.random.split(jax.random.fold_in(keys[5], 1), TOKENS // TOK_DEV)
    expert_ids_turns = jax.random.permutation(jax.random.fold_in(keys[5], 3), TOKENS // TOK_DEV)
    expert_ids = jax.vmap(lambda own, number: deal_out(jax.random.fold_in(keys[5], 2), own, number, TOK_DEV, EXPERTS, TOPK, CAP, 2))(expert_ids_keys, expert_ids_turns).reshape((TOKENS, TOPK))
    route_weight = jnp.clip(0.2 + 0.8 * jax.random.uniform(keys[6], (TOKENS, TOPK), jnp.float32) ** level_of(keys[6], (TOKENS, TOPK), ((0, 8),), -0.2, 0.2), 0.2, 1.0)
    return {"tokens": tokens, "norm_gain": norm_gain, "gate_weight": gate_weight, "up_weight": up_weight, "down_weight": down_weight, "expert_ids": expert_ids, "route_weight": route_weight}


epsilon = 1e-06
swish_alpha = 1.702
clamp_limit = 7.0

def rms_normed(values, norm_gain):
    widened = values.astype(jnp.float32)
    scaled = widened * lax.rsqrt(lax.optimization_barrier(jnp.mean(widened * widened, axis=-1, keepdims=True)) + epsilon)
    return (scaled * norm_gain.astype(jnp.float32)).astype(jnp.bfloat16)

def slot_numbers(flat_ids, expert_count):
    selector = (flat_ids[..., None] == jnp.arange(expert_count, dtype=jnp.int32)).astype(jnp.int32)
    before = jnp.cumsum(selector, axis=-2) - selector
    return lax.optimization_barrier(jnp.sum(before * selector, axis=-1)).astype(jnp.int32)

def clamped_units(row_block, w_gate, w_up, w_down):
    gate_pre = jnp.dot(row_block, w_gate, preferred_element_type=jnp.float32)
    up_pre = jnp.dot(row_block, w_up, preferred_element_type=jnp.float32)
    gate_pre = jnp.minimum(gate_pre, clamp_limit)
    up_pre = jnp.clip(up_pre, -clamp_limit, clamp_limit)
    hidden = ((up_pre + 1.0) * gate_pre * jax.nn.sigmoid(swish_alpha * gate_pre)).astype(jnp.bfloat16)
    return jnp.dot(hidden, w_down, preferred_element_type=jnp.float32).astype(jnp.bfloat16)

def reference(tokens, norm_gain, gate_weight, up_weight, down_weight, expert_ids, route_weight):
    normed = rms_normed(tokens, norm_gain)
    assigned = TOK_DEV * TOPK
    flat_ids = expert_ids.reshape(N_EP, assigned).astype(jnp.int32)
    slot_index = slot_numbers(flat_ids, EXPERTS)
    source = jnp.broadcast_to(jnp.arange(N_EP, dtype=jnp.int32)[:, None], (N_EP, assigned))
    owner_token = source * TOK_DEV + jnp.arange(assigned, dtype=jnp.int32)[None, :] // TOPK
    slot_table = jnp.full((EXPERTS, N_EP, CAP), TOKENS, jnp.int32).at[flat_ids, source, slot_index].set(owner_token)
    padded = jnp.concatenate([normed, jnp.zeros((1, D), jnp.bfloat16)], axis=0)

    def one_expert(packed):
        index_table, w_gate, w_up, w_down = packed
        return clamped_units(padded[index_table.reshape(-1)], w_gate, w_up, w_down)
    results = lax.map(one_expert, (slot_table, gate_weight, up_weight, down_weight))
    flat_results = results.reshape(EXPERTS * N_EP * CAP, D)
    locator = ((flat_ids * N_EP + source) * CAP + slot_index).reshape(TOKENS, TOPK)
    picked = flat_results[locator].astype(jnp.float32)
    combined = lax.optimization_barrier(jnp.sum(picked * route_weight.astype(jnp.float32)[:, :, None], axis=1))
    return combined.astype(jnp.bfloat16)
```

```python
import functools

import jax
import jax.numpy as jnp
from jax import lax
from jax.experimental import pallas as pl
from jax.experimental.pallas import tpu as pltpu
from jax.sharding import PartitionSpec as P

epsilon = 1e-06
swish_alpha = 1.702
clamp_limit = 7.0


def over_all(shard, axis, dim, take_in, carry):
    whole = jax.tree.map(lambda part: lax.all_gather(part, axis, axis=dim, tiled=True), shard)
    return take_in(carry, whole, jnp.int32(0))


def rms_normed(values, norm_gain):
    widened = values.astype(jnp.float32)
    scaled = widened * lax.rsqrt(jnp.mean(widened * widened, axis=-1, keepdims=True) + epsilon)
    return (scaled * norm_gain.astype(jnp.float32)).astype(jnp.bfloat16)


def slot_numbers(flat_ids, expert_count):
    selector = (flat_ids[..., None] == jnp.arange(expert_count, dtype=jnp.int32)).astype(jnp.int32)
    before = jnp.cumsum(selector, axis=-2) - selector
    return jnp.sum(before * selector, axis=-1).astype(jnp.int32)


def by_expert(incoming, ep_count, local_experts):
    capacity = incoming.shape[1]
    width = incoming.shape[2]
    grouped = incoming.reshape(ep_count, local_experts, capacity, width)
    return jnp.transpose(grouped, (1, 0, 2, 3)).reshape(local_experts, ep_count * capacity, width)


def body(tokens, norm_gain, gate_weight, up_weight, down_weight, expert_ids, route_weight):
    tok_rows = expert_ids.shape[0]
    top_count = expert_ids.shape[1]
    local_experts = gate_weight.shape[0]
    ep_count = lax.axis_size("ep")
    expert_total = local_experts * ep_count
    capacity = 2 * tok_rows * top_count // expert_total
    out_width = down_weight.shape[2]
    flat_ids = expert_ids.reshape(-1).astype(jnp.int32)
    slot_index = slot_numbers(flat_ids, expert_total)
    owner_token = jnp.arange(tok_rows * top_count, dtype=jnp.int32) // top_count
    slot_table = (
        jnp.full((expert_total, capacity), tok_rows, jnp.int32)
        .at[flat_ids, slot_index]
        .set(owner_token)
    )
    whole = lax.all_gather(tokens, "tp", axis=1, tiled=True)
    normed = rms_normed(whole, norm_gain)
    width = normed.shape[1]
    padded = jnp.concatenate([normed, jnp.zeros((1, width), jnp.bfloat16)], axis=0)
    outgoing = padded[slot_table.reshape(-1)].reshape(expert_total, capacity, width)
    incoming = lax.all_to_all(outgoing, "ep", split_axis=0, concat_axis=0, tiled=True)
    row_block = by_expert(incoming, ep_count, local_experts)
    gate_pre = jnp.einsum(
        "esd,edf->esf", row_block, gate_weight, preferred_element_type=jnp.float32
    )
    up_pre = jnp.einsum("esd,edf->esf", row_block, up_weight, preferred_element_type=jnp.float32)
    gate_pre = jnp.minimum(gate_pre, clamp_limit)
    up_pre = jnp.clip(up_pre, -clamp_limit, clamp_limit)
    hidden = ((up_pre + 1.0) * gate_pre * jax.nn.sigmoid(swish_alpha * gate_pre)).astype(
        jnp.bfloat16
    )
    empty_out = jnp.zeros((local_experts, ep_count * capacity, out_width), jnp.float32)

    def add_hidden(total, piece, start):
        down_rows = lax.dynamic_slice_in_dim(down_weight, start, piece.shape[2], 1)
        return total + jnp.einsum(
            "esf,efd->esd", piece, down_rows, preferred_element_type=jnp.float32
        )

    down_sum = over_all(hidden, "tp", 2, add_hidden, empty_out)
    expert_out = down_sum.astype(jnp.bfloat16).reshape(local_experts, ep_count, capacity, out_width)
    sendback = jnp.transpose(expert_out, (1, 0, 2, 3)).reshape(
        ep_count * local_experts, capacity, out_width
    )
    returned = lax.all_to_all(sendback, "ep", split_axis=0, concat_axis=0, tiled=True)
    flat_back = returned.reshape(expert_total * capacity, out_width)
    picked = (
        flat_back[flat_ids * capacity + slot_index]
        .reshape(tok_rows, top_count, out_width)
        .astype(jnp.float32)
    )
    combined = jnp.sum(picked * route_weight.astype(jnp.float32)[:, :, None], axis=1)
    return combined.astype(jnp.bfloat16)


MESH = pl.DeviceIdType.MESH


def fused_kernel(
    nz,
    gain_ref,
    ids_ref,
    route_ref,
    tok_ref,
    gw_ref,
    uw_ref,
    dw_ref,
    out_ref,
    xbuf,
    gw,
    uw,
    wd,
    nbuf,
    wbuf,
    keep,
    dsend,
    drecv,
    r1send,
    r1recv,
    r2send,
    r2recv,
    zsend,
    zrecv,
    near,
    lsem,
    wd_s,
    wd_r,
    w_s,
    w_r,
    az_s,
    az_r,
    ax_s,
    ax_r,
    af_s,
    af_r,
    ac_s,
    ac_r,
    d_s,
    d_r,
    r1_s,
    r1_r,
    r2_s,
    r2_r,
    z_s,
    z_r,
):
    ep, tp = lax.axis_index("ep"), lax.axis_index("tp")
    rows, part = xbuf.shape[3], xbuf.shape[4]
    half = rows // 2
    width = 4 * part

    def dev(zc, r):
        return (lax.bitwise_xor(ep, zc), lax.bitwise_xor(tp, r))

    def remote(src, dst, s_sem, r_sem, zc, r):
        return pltpu.make_async_remote_copy(
            src_ref=src,
            dst_ref=dst,
            send_sem=s_sem,
            recv_sem=r_sem,
            device_id=dev(zc, r),
            device_id_type=MESH,
        )

    def quarter(r):
        return pl.ds(pl.multiple_of(lax.bitwise_xor(tp, r) * part, part), part)

    local = [pltpu.make_async_copy(tok_ref, xbuf.at[0, 0, 0], lsem.at[0])]
    for r in range(4):
        here = pl.ds(r * part, part)
        local.append(pltpu.make_async_copy(gw_ref.at[0, quarter(r)], gw.at[here], lsem.at[1 + r]))
        local.append(pltpu.make_async_copy(uw_ref.at[0, quarter(r)], uw.at[here], lsem.at[5 + r]))
    local.append(pltpu.make_async_copy(dw_ref.at[0, quarter(0)], wd.at[0], lsem.at[9]))
    for copy in local:
        copy.start()

    barrier = pltpu.get_barrier_semaphore()
    for zc in range(1, 2 * nz):
        pl.semaphore_signal(barrier, inc=1, device_id=dev(zc, 0), device_id_type=MESH)
    for r in range(1, 4):
        pl.semaphore_signal(barrier, inc=1, device_id=dev(0, r), device_id_type=MESH)

    lane = lax.broadcasted_iota(jnp.int32, (rows, 128), 1)
    dense = jnp.zeros((rows, 128), jnp.float32)
    for k in range(ids_ref.shape[1]):
        dense = dense + jnp.where(ids_ref[:, k : k + 1] == lane, route_ref[:, k : k + 1], 0.0)
    wbuf[0] = dense.T[: 2 * nz]

    local[0].wait()
    pl.semaphore_wait(barrier, 2 * nz + 2)

    started = []

    def go(copy):
        copy.start()
        started.append(copy)
        return copy

    az = {}
    for s in range(1, nz):
        az[s] = go(remote(xbuf.at[0, 0, 0], xbuf.at[s, 0, 0], az_s.at[s], az_r.at[s], 2 * s, 0))
    ax, af, ac = {}, {}, {}

    def spread(s):
        for r in (1, 2):
            ax[s, r] = go(
                remote(xbuf.at[s, 0, 0], xbuf.at[s, 0, r], ax_s.at[s, r], ax_r.at[s, r], 0, r)
            )
        share(s, 0)

    def share(s, r):
        ac[s, r] = go(
            remote(xbuf.at[s, 0, r], xbuf.at[s, 1, r], ac_s.at[s, r], ac_r.at[s, r], 1, 0)
        )

    def pass_on(s):
        for r, to in ((1, 2), (2, 1)):
            ax[s, r].wait_recv()
            piece = pl.ds((r - 1) * half, half)
            af[s, r] = go(
                remote(
                    xbuf.at[s, 0, r, piece],
                    xbuf.at[s, 0, 3, piece],
                    af_s.at[s, r],
                    af_r.at[s, r],
                    0,
                    to,
                )
            )
            share(s, r)

    def finish_gather(s):
        af[s, 1].wait_recv()
        af[s, 2].wait_recv()
        share(s, 3)
        for r in range(4):
            ac[s, r].wait_recv()

    spread(0)
    w_copies = [
        go(remote(wbuf.at[0], wbuf.at[zc], w_s.at[zc], w_r.at[zc], zc, 0))
        for zc in range(1, 2 * nz)
    ]
    wd_copies = [
        go(
            remote(dw_ref.at[0, quarter(r)], wd.at[r], wd_s.at[r], wd_r.at[r], 0, r)
        )
        for r in range(1, 4)
    ]

    def compute(s):
        for cr in range(2):
            parts = [xbuf[s, cr, r].astype(jnp.float32) for r in range(4)]
            square = parts[0] * parts[0]
            for p in parts[1:]:
                square = square + p * p
            scale = lax.rsqrt(jnp.sum(square, axis=-1, keepdims=True) / width + epsilon)
            for r in range(4):
                gain = gain_ref[pl.ds(lax.bitwise_xor(tp, r), 1), :]
                nbuf[pl.ds(cr * rows, rows), pl.ds(r * part, part)] = (
                    parts[r] * scale * gain
                ).astype(jnp.bfloat16)
        g = jnp.dot(nbuf[...], gw[...], preferred_element_type=jnp.float32)
        u = jnp.dot(nbuf[...], uw[...], preferred_element_type=jnp.float32)
        g = jnp.minimum(g, clamp_limit)
        u = jnp.clip(u, -clamp_limit, clamp_limit)
        return ((u + 1.0) * g * jax.nn.sigmoid(swish_alpha * g)).astype(jnp.bfloat16)

    def down(s, hidden):
        scales = []
        for cr in range(2):
            line = wbuf[2 * s + cr, pl.ds(ep, 1), :]
            column = jnp.broadcast_to(line, (rows, rows)).T
            scales.append(jnp.concatenate([column] * (part // rows), axis=1))
        for r in range(4):
            full = jnp.dot(hidden, wd[r], preferred_element_type=jnp.float32)
            keep[s, r] = full[:rows] * scales[0]
            dsend[s, r] = full[rows:] * scales[1]
        return go(remote(dsend.at[s], drecv.at[s], d_s.at[s], d_r.at[s], 1, 0))

    d, r1, r2, zc_copies = {}, {}, {}, {}

    def reduce_one(s):
        d[s].wait_recv()
        total = [keep[s, r] + drecv[s, r] for r in range(4)]
        r1send[s, 0, 0] = total[1][:half].astype(jnp.bfloat16)
        r1send[s, 0, 1] = total[3][:half].astype(jnp.bfloat16)
        r1send[s, 1, 0] = total[2][half:].astype(jnp.bfloat16)
        r1send[s, 1, 1] = total[3][half:].astype(jnp.bfloat16)
        for h in range(2):
            r1[s, h] = go(
                remote(r1send.at[s, h], r1recv.at[s, h], r1_s.at[s, h], r1_r.at[s, h], 0, 1 + h)
            )
        keep[s, 0] = total[0]
        keep[s, 1, half:] = total[1][half:]
        keep[s, 2, :half] = total[2][:half]

    def reduce_two(s):
        for h in range(2):
            r1[s, h].wait_recv()
            piece = pl.ds(h * half, half)
            r2send[s, h] = keep[s, 2 - h, piece] + r1recv[s, h, 1].astype(jnp.float32)
            r2[s, h] = go(
                remote(r2send.at[s, h], r2recv.at[s, h], r2_s.at[s, h], r2_r.at[s, h], 0, 2 - h)
            )

    def reduce_three(s):
        for h in range(2):
            r2[s, h].wait_recv()
            piece = pl.ds(h * half, half)
            value = (
                keep[s, 0, piece]
                + r1recv[s, h, 0].astype(jnp.float32)
                + r2recv[s, h]
            )
            if s == 0:
                keep[s, 0, piece] = value
            elif s == 1:
                near[0, piece] = value
            else:
                zsend[s, piece] = value.astype(jnp.bfloat16)
        if s:
            out, into = (near.at[0], near.at[1]) if s == 1 else (zsend.at[s], zrecv.at[s])
            zc_copies[s] = go(remote(out, into, z_s.at[s], z_r.at[s], 2 * s, 0))

    for s in range(nz):
        if s + 1 < nz:
            az[s + 1].wait_recv()
            spread(s + 1)
        pass_on(s)
        finish_gather(s)
        if s == 0:
            for copy in local[1:]:
                copy.wait()
        hidden = compute(s)
        if s == 0:
            for copy in wd_copies + w_copies:
                copy.wait_recv()
        d[s] = down(s, hidden)
        if s >= 1:
            reduce_one(s - 1)
        if s >= 2:
            reduce_two(s - 2)
        if s >= 3:
            reduce_three(s - 3)
    for s in range(nz, nz + 3):
        if s - 1 < nz:
            reduce_one(s - 1)
        if 0 <= s - 2 < nz:
            reduce_two(s - 2)
        if 0 <= s - 3 < nz:
            reduce_three(s - 3)
    result = keep[0, 0]
    for s in range(1, nz):
        zc_copies[s].wait_recv()
        result = result + (near[1] if s == 1 else zrecv[s].astype(jnp.float32))
    out_ref[...] = result.astype(jnp.bfloat16)
    for copy in started:
        copy.wait_send()


def fused_body(
    nz, tokens, norm_gain, gate_weight, up_weight, down_weight, expert_ids, route_weight
):
    rows, part = tokens.shape
    half = rows // 2
    width = gate_weight.shape[1]
    units = gate_weight.shape[2]
    dma = pltpu.SemaphoreType.DMA
    vmem = pl.BlockSpec(memory_space=pltpu.VMEM)
    anywhere = pl.BlockSpec(memory_space=pl.ANY)
    bf, f32 = jnp.bfloat16, jnp.float32
    return pl.pallas_call(
        functools.partial(fused_kernel, nz),
        out_shape=jax.ShapeDtypeStruct((rows, part), bf),
        in_specs=[vmem] * 3 + [anywhere] * 4,
        out_specs=vmem,
        scratch_shapes=[
            pltpu.VMEM((nz, 2, 4, rows, part), bf),
            pltpu.VMEM((width, units), bf),
            pltpu.VMEM((width, units), bf),
            pltpu.VMEM((4, units, part), bf),
            pltpu.VMEM((2 * rows, width), bf),
            pltpu.VMEM((2 * nz, 2 * nz, rows), f32),
            pltpu.VMEM((nz, 4, rows, part), f32),
            pltpu.VMEM((nz, 4, rows, part), f32),
            pltpu.VMEM((nz, 4, rows, part), f32),
            pltpu.VMEM((nz, 2, 2, half, part), bf),
            pltpu.VMEM((nz, 2, 2, half, part), bf),
            pltpu.VMEM((nz, 2, half, part), f32),
            pltpu.VMEM((nz, 2, half, part), f32),
            pltpu.VMEM((nz, rows, part), bf),
            pltpu.VMEM((nz, rows, part), bf),
            pltpu.VMEM((2, rows, part), f32),
            dma((10,)),
            dma((4,)),
            dma((4,)),
            dma((2 * nz,)),
            dma((2 * nz,)),
            dma((nz,)),
            dma((nz,)),
            dma((nz, 3)),
            dma((nz, 3)),
            dma((nz, 3)),
            dma((nz, 3)),
            dma((nz, 4)),
            dma((nz, 4)),
            dma((nz,)),
            dma((nz,)),
            dma((nz, 2)),
            dma((nz, 2)),
            dma((nz, 2)),
            dma((nz, 2)),
            dma((nz,)),
            dma((nz,)),
        ],
        compiler_params=pltpu.CompilerParams(
            collective_id=0, has_side_effects=True, vmem_limit_bytes=48 * 1024 * 1024
        ),
    )(
        norm_gain.reshape(4, part),
        expert_ids,
        route_weight,
        tokens,
        gate_weight,
        up_weight,
        down_weight,
    )


def chosen(tokens, norm_gain, gate_weight, up_weight, down_weight, expert_ids, route_weight):
    args = (tokens, norm_gain, gate_weight, up_weight, down_weight, expert_ids, route_weight)
    ep_count, tp_count = lax.axis_size("ep"), lax.axis_size("tp")
    rows, part = tokens.shape
    units = gate_weight.shape[2]
    nz = ep_count // 2
    fits = (
        tp_count == 4
        and nz >= 2
        and nz & (nz - 1) == 0
        and nz <= 4
        and ep_count % 8 == 0
        and gate_weight.shape[0] == 1
        and rows == 128
        and part % 128 == 0
        and units == part
        and down_weight.shape[2] == part
    )
    if not fits:
        return body(*args)
    return fused_body(nz, *args)


def solution(mesh):
    in_specs = (
        P("ep", "tp"),
        P(),
        P("ep", None, "tp"),
        P("ep", None, "tp"),
        P("ep", None, "tp"),
        P("ep", None),
        P("ep", None),
    )
    out_specs = P("ep", "tp")
    return jax.shard_map(chosen, mesh=mesh, in_specs=in_specs, out_specs=out_specs, check_vma=False)
```
